32 devices in a mesh: sp: 8 (over z, y), tp: 4 (over x, core).
Axes of the slice: x: 2, y: 2, z: 4, core: 2. Of those that a mesh axis runs over, the one named last changes fastest.
Arguments:
- residual_in: bfloat16 [16384, 2048], P(('sp', 'tp')), may hold values from -6 to 6
- conv_input: bfloat16 [16384, 1024], P('sp', 'tp'), may hold values from -6 to 6
- input_gate: bfloat16 [16384, 1024], P('sp', 'tp'), may hold values from -6 to 6
- output_gate: bfloat16 [16384, 1024], P('sp', 'tp'), may hold values from -6 to 6
- conv_taps: bfloat16 [3, 1024], P(None, 'tp'), may hold values from -3.5 to 3.5
- doc_ids: int32 [16384], P('sp'), may hold values from 0 to 3, never falling along the last dimension, each value on 1 to 8192 neighbouring positions
- proj_weight: bfloat16 [1024, 2048], replicated, may hold values from -0.1875 to 0.1875
- norm_gain: float32 [2048], replicated, may hold values from 0.1 to 1.9
- expert_ids: int32 [16384, 2], P(('sp', 'tp')), may hold values from 0 to 31, all different within a row; in each aligned block of 512 rows (0 to 511, 512 to 1023, ...) at most 64 rows name the same one
- expert_weight: float32 [16384, 2], P(('sp', 'tp')), may hold values from 0.05 to 1
- w_gate: bfloat16 [32, 2048, 512], P('sp'), may hold values from -0.125 to 0.125
- w_up: bfloat16 [32, 2048, 512], P('sp'), may hold values from -0.125 to 0.125
- w_down: bfloat16 [32, 512, 2048], P('sp'), may hold values from -0.25 to 0.25
Outputs:
- layer_out: bfloat16 [16384, 2048], P(('sp', 'tp'))
The draws below stay inside these ranges and needn't reach their ends.
Inputs may be any that keep to these rules, and one draw needn't show every extreme that they name: `doc_ids`: numbers never fall along the sequence; one document spans at most 8192 positions. `expert_ids`: a token's two experts differ; in each aligned block of rows that one device holds, no expert is named more than 64 times, a bound that some block reaches.
All inputs are finite; a program needn't handle non-finite values.
Results may differ from the reference program's by a relative error of at most 0.0047.
Values may be sent and summed in bfloat16 or wider, within the bound.
A program may use at most 128 MiB of HBM per device.

```python
import math
import jax
import jax.numpy as jnp
import numpy as np
from jax import lax

D = 2048
CONV = 1024
FFE = 512
EXPERTS = 32
KW = 3
CAP = 64
TOK_DEV = 2048
TOKENS = 16384
SEG_COUNT = 4
DOC_MOST = 8192
N_SP = 8
N_TP = 4


def block_scale(rng, dims, cuts, smallest, high):
    def one(dim, parts):
        heights = jax.random.uniform(jax.random.fold_in(jax.random.fold_in(rng, 6), dim), (parts,), jnp.float32, smallest / len(cuts), high / len(cuts))
        return jnp.repeat(jnp.exp(heights), dims[dim] // parts).reshape((-1,) + (1,) * (len(dims) - dim - 1))

    loudness = one(*cuts[0])
    for cut in cuts[1:]:
        loudness = loudness * one(*cut)
    return loudness


def profile(amount, total, limit, skew):
    loads = [(1 << 20) // math.isqrt(grade ** skew) + 1 for grade in range(2, amount + 1)]
    surplus, holding = total - limit - (amount - 1), [1] * (amount - 1)
    while surplus > 0:
        free = [i for i in range(amount - 1) if holding[i] < limit]
        mass, budget = sum([loads[i] for i in free]), surplus
        for i in free:
            more = min(limit - holding[i], max(1, budget * loads[i] // mass), surplus)
            holding[i] = holding[i] + more
            surplus = surplus - more
    return np.array([limit] + holding)


def ragged_sizes(stream_key, number_of, total, reach, skew):
    if number_of == 2:
        one = jax.random.randint(stream_key, (), max(1, total - reach), min(reach, total - 1) + 1)
        return jnp.stack([one, total - one])
    sizes = jnp.asarray(profile(number_of, total, reach, skew), jnp.int32)
    couples = (number_of - 1) // 2
    giver, receiver = sizes[1:1 + 2 * couples:2], sizes[2:2 + 2 * couples:2]
    room = jnp.minimum(giver - 1, reach - receiver)
    moved = jax.random.randint(jax.random.fold_in(stream_key, 1), (couples,), 0, 1 << 20) % (room + 1)
    sizes = sizes.at[1:1 + 2 * couples:2].set(giver - moved).at[2:2 + 2 * couples:2].set(receiver + moved)
    return sizes[jax.random.permutation(jax.random.fold_in(stream_key, 2), number_of)]


def assign_block(rng, own, number, rows, number_of, top, bound, lean):
    ranking = jax.random.permutation(rng, number_of)
    packed, common = shares(number_of, rows * top, bound, lean, True), shares(number_of, rows * top, bound, lean, False)
    places = jnp.arange(number_of)

    def named(sizes, turn):
        used = int((sizes > 0).sum())
        fixed = max(1, used // 4)
        passed = fixed + (places - fixed + turn * (used - fixed)) % max(1, number_of - fixed)
        return jnp.zeros((number_of,), jnp.int32).at[ranking[jnp.where(places < fixed, places, passed)]].set(jnp.asarray(sizes, jnp.int32))

    sizes = jnp.where(number % 4 == 0, named(packed, number // 4), named(common, number - number // 4 - 1))
    mixed = jax.random.permutation(jax.random.fold_in(own, 3), number_of)
    donor, taker = mixed[0:number_of // 2 * 2:2], mixed[1:number_of // 2 * 2:2]
    slack = jnp.minimum(sizes[donor] - 1, bound - sizes[taker]) // 2
    slack = jnp.where((donor == ranking[0]) | (taker == ranking[0]) | (sizes[taker] == 0), 0, jnp.maximum(slack, 0))
    passed = jax.random.randint(jax.random.fold_in(own, 4), (number_of // 2,), 0, 1 << 20) % (slack + 1)
    sizes = sizes.at[donor].add(-passed).at[taker].add(passed)
    labels = jnp.searchsorted(jnp.cumsum(sizes), jnp.arange(rows * top), side="right").astype(jnp.int32)
    listing = labels.reshape(top, rows).T
    listing = listing[jax.random.permutation(jax.random.fold_in(own, 1), rows)]
    turn = jax.random.randint(jax.random.fold_in(own, 2), (rows, 1), 0, top)
    return jnp.take_along_axis(listing, (jnp.arange(top)[None, :] + turn) % top, axis=1)


def shares(amount, total, most, skew, full):
    weights = [(1 << 20) // math.isqrt(standing ** skew) + 1 for standing in range(1, amount + 1)]
    largest = most if full else min(most, max(-(-total // amount), total * weights[0] // sum(weights)))
    least = 1 if total - largest >= amount - 1 else 0
    counts, spare = [largest] + [least] * (amount - 1), total - largest - least * (amount - 1)
    while spare > 0:
        movable = [i for i in range(1, amount) if counts[i] < largest] or [i for i in range(1, amount) if counts[i] < most]
        mass, budget = sum([weights[i] for i in movable]), spare
        for i in movable:
            addition = min(most - counts[i], max(1, budget * weights[i] // mass), spare)
            counts[i] = counts[i] + addition
            spare = spare - addition
    return np.array(counts)


def centred(rng, extent, width, most, split=(), kind=jnp.bfloat16):
    values = width * jax.random.normal(rng, extent, jnp.float32)
    if split:
        values = values * block_scale(rng, extent, split, -0.22, 0.18)
    return jnp.clip(values, -most, most).astype(kind)


def setup_inputs(seed: int = 0) -> dict:
    key_of = jax.random.split(jax.random.key(seed), 14)
    residual_in = centred(key_of[0], (TOKENS, D), 1.0, 6.0, ((0, 32),))
    conv_input = centred(key_of[1], (TOKENS, CONV), 1.0, 6.0, ((0, 8), (1, 4)))
    input_gate = centred(key_of[2], (TOKENS, CONV), 1.0, 6.0, ((0, 8), (1, 4)))
    output_gate = centred(key_of[3], (TOKENS, CONV), 1.0, 6.0, ((0, 8), (1, 4)))
    conv_taps = centred(key_of[4], (KW, CONV), KW ** -0.5, 3.5, ((1, 4),))
    doc_ids = jnp.searchsorted(jnp.cumsum(ragged_sizes(key_of[5], SEG_COUNT, TOKENS, DOC_MOST, 2)), jnp.arange(TOKENS), side="right").astype(jnp.int32)
    proj_weight = centred(key_of[6], (CONV, D), CONV ** -0.5, 0.1875)
    norm_gain = jnp.clip(1.0 + 0.18 * jax.random.normal(key_of[7], (D,), jnp.float32), 0.1, 1.9)
    expert_ids_keys = jax.random.split(jax.random.fold_in(key_of[8], 1), TOKENS // (TOK_DEV // N_TP))
    expert_ids_turns = jax.random.permutation(jax.random.fold_in(key_of[8], 3), TOKENS // (TOK_DEV // N_TP))
    expert_ids = jax.vmap(lambda own, number: assign_block(jax.random.fold_in(key_of[8], 2), own, number, TOK_DEV // N_TP, EXPERTS, 2, CAP, 2))(expert_ids_keys, expert_ids_turns).reshape((TOKENS, 2))
    expert_weight = jnp.clip(jnp.exp(math.log(1.0) - 2.9957323 * jax.random.uniform(key_of[9], (TOKENS, 2), jnp.float32) ** block_scale(key_of[9], (TOKENS, 2), ((0, 32),), -0.2, 0.2)), 0.05, 1.0)
    w_gate = centred(key_of[10], (EXPERTS, D, FFE), D ** -0.5, 0.125, ((0, 8),))
    w_up = centred(key_of[11], (EXPERTS, D, FFE), D ** -0.5, 0.125, ((0, 8),))
    w_down = centred(key_of[12], (EXPERTS, FFE, D), FFE ** -0.5, 0.25, ((0, 8),))
    return dict(residual_in=residual_in, conv_input=conv_input, input_gate=input_gate, output_gate=output_gate, conv_taps=conv_taps, doc_ids=doc_ids, proj_weight=proj_weight, norm_gain=norm_gain, expert_ids=expert_ids, expert_weight=expert_weight, w_gate=w_gate, w_up=w_up, w_down=w_down)


epsilon = 1e-06

def reference(residual_in, conv_input, input_gate, output_gate, conv_taps, doc_ids, proj_weight, norm_gain, expert_ids, expert_weight, w_gate, w_up, w_down):
    product = input_gate.astype(jnp.float32) * conv_input.astype(jnp.float32)
    padded_in = jnp.concatenate([jnp.zeros((KW - 1, CONV), jnp.float32), product], axis=0)
    padded_ids = jnp.concatenate([jnp.full((KW - 1,), -1, jnp.int32), doc_ids.astype(jnp.int32)], axis=0)
    conv_sum = jnp.zeros((TOKENS, CONV), jnp.float32)
    for offset in range(KW):
        same_doc = padded_ids[offset:offset + TOKENS] == doc_ids
        term = conv_taps[offset].astype(jnp.float32)[None, :] * padded_in[offset:offset + TOKENS]
        conv_sum = conv_sum + jnp.where(same_doc[:, None], term, 0.0)
    gated = (output_gate.astype(jnp.float32) * conv_sum).astype(jnp.bfloat16)
    hidden = residual_in.astype(jnp.float32) + jnp.dot(gated, proj_weight, preferred_element_type=jnp.float32)
    scale_rows = lax.rsqrt(lax.optimization_barrier(jnp.mean(hidden * hidden, axis=-1, keepdims=True)) + epsilon)
    normed = (hidden * scale_rows * norm_gain[None, :]).astype(jnp.bfloat16)
    blocks = N_SP * N_TP
    block_rows = TOK_DEV // N_TP
    slots_all = blocks * CAP
    flat_ids = expert_ids.reshape(blocks, 2 * block_rows)
    one_hot = (flat_ids[:, :, None] == jnp.arange(EXPERTS, dtype=jnp.int32)[None, None, :]).astype(jnp.int32)
    before = jnp.cumsum(one_hot, axis=1) - one_hot
    slot_num = lax.optimization_barrier(jnp.sum(before * one_hot, axis=-1))
    slot_index = (jnp.arange(blocks, dtype=jnp.int32)[:, None] * CAP + slot_num).reshape(TOKENS, 2).astype(jnp.int32)

    def per_expert(total, expert):
        chosen = expert_ids == expert
        target = jnp.where(chosen, slot_index, slots_all)
        buffer = jnp.zeros((slots_all, D), jnp.bfloat16)
        buffer = buffer.at[target[:, 0]].set(normed, mode='drop')
        buffer = buffer.at[target[:, 1]].set(normed, mode='drop')
        gate_val = jnp.dot(buffer, w_gate[expert], preferred_element_type=jnp.float32)
        up_val = jnp.dot(buffer, w_up[expert], preferred_element_type=jnp.float32)
        act_rows = (jax.nn.silu(gate_val) * up_val).astype(jnp.bfloat16)
        out_rows = jnp.dot(act_rows, w_down[expert], preferred_element_type=jnp.float32).astype(jnp.bfloat16)
        for route in range(2):
            picked = out_rows[slot_index[:, route]].astype(jnp.float32) * expert_weight[:, route:route + 1]
            total = total + jnp.where(chosen[:, route:route + 1], picked, 0.0)
        return (total, None)
    expert_sum, unused = lax.scan(per_expert, jnp.zeros((TOKENS, D), jnp.float32), jnp.arange(EXPERTS, dtype=jnp.int32))
    return (hidden + expert_sum).astype(jnp.bfloat16)
```

```python
import functools

import jax
import jax.numpy as jnp
from jax import lax
from jax.experimental import pallas as pl
from jax.experimental.pallas import tpu as pltpu
from jax.sharding import PartitionSpec as P

CAP = 64
CHUNKS = 2
epsilon = 1e-06


def from_behind(x, axis, by):
    devices = lax.axis_size(axis)
    pairs = [(i, i + by) for i in range(devices) if 0 <= i + by < devices]
    return lax.ppermute(x, axis, pairs)


def to_mirror(x):
    devices = lax.axis_size("sp")
    pairs = [(i, (i + devices // 2) % devices) for i in range(devices)]
    return lax.ppermute(x, "sp", pairs)


def within_half(x):
    devices = lax.axis_size("sp")
    half = devices // 2
    groups = [list(range(half)), list(range(half, devices))]
    return lax.all_to_all(x, "sp", split_axis=0, concat_axis=0, axis_index_groups=groups, tiled=True)


def ffn_kernel(chunks, *refs):
    x_refs = refs[:chunks]
    gate_ref, up_ref, down_ref = refs[chunks : chunks + 3]
    out_refs = refs[chunks + 3 :]
    peers, cap, width = x_refs[0].shape
    gate_val, up_val = 0.0, 0.0
    for c in range(chunks):
        rows = x_refs[c][...].reshape(peers * cap, width)
        part = pl.ds(c * width, width)
        gate_val = gate_val + jnp.dot(rows, gate_ref[part, :], preferred_element_type=jnp.float32)
        up_val = up_val + jnp.dot(rows, up_ref[part, :], preferred_element_type=jnp.float32)
    act = (gate_val * jax.nn.sigmoid(gate_val) * up_val).astype(jnp.bfloat16)
    for c in range(chunks):
        part = pl.ds(c * width, width)
        out = jnp.dot(act, down_ref[:, part], preferred_element_type=jnp.float32)
        out_refs[c][...] = out.astype(jnp.bfloat16).reshape(peers, cap, width)


def expert_ffn(xs, w_gate, w_up, w_down):
    chunks = len(xs)
    peers, experts, cap, width = xs[0].shape
    model, hidden = w_gate.shape[1:]
    row_spec = pl.BlockSpec((peers, None, cap, width), lambda e: (0, e, 0, 0))
    return pl.pallas_call(
        functools.partial(ffn_kernel, chunks),
        grid=(experts,),
        in_specs=[row_spec] * chunks
        + [
            pl.BlockSpec((None, model, hidden), lambda e: (e, 0, 0)),
            pl.BlockSpec((None, model, hidden), lambda e: (e, 0, 0)),
            pl.BlockSpec((None, hidden, model), lambda e: (e, 0, 0)),
        ],
        out_specs=[row_spec] * chunks,
        out_shape=[jax.ShapeDtypeStruct(xs[0].shape, jnp.bfloat16)] * chunks,
        cost_estimate=pl.CostEstimate(
            flops=6 * experts * peers * cap * model * hidden,
            bytes_accessed=2 * (w_gate.size + w_up.size + w_down.size + 2 * chunks * xs[0].size),
            transcendentals=experts * peers * cap * hidden,
        ),
    )(*xs, w_gate, w_up, w_down)


def slot_matrices(ids, weights, first, experts):
    tokens = ids.shape[1]
    local = ids - first
    names = jnp.arange(experts, dtype=jnp.int32)[:, None]
    hits = [local[r][None, :] == names for r in range(2)]
    named = (hits[0] | hits[1]).astype(jnp.bfloat16)
    at = jnp.arange(tokens, dtype=jnp.int32)
    earlier = (at[:, None] < at[None, :]).astype(jnp.bfloat16)
    before = jnp.dot(named, earlier, preferred_element_type=jnp.float32)
    slots = jnp.arange(experts * CAP, dtype=jnp.int32)[:, None]
    pick, mix = False, 0.0
    for r in range(2):
        rank = jnp.sum(jnp.where(hits[r], before, 0.0), axis=0).astype(jnp.int32)
        match = slots == (local[r] * CAP + rank)[None, :]
        pick = pick | match
        mix = mix + jnp.where(match, weights[r][None, :], 0.0)
    return pick.astype(jnp.bfloat16), mix.astype(jnp.bfloat16)


def pack(pick, rows, peers, experts):
    out = jnp.dot(pick, rows, preferred_element_type=jnp.float32).astype(jnp.bfloat16)
    return out.reshape(peers, experts, CAP, rows.shape[1])


def unpack(mix, returned):
    flat = returned.reshape(-1, returned.shape[-1])
    return lax.dot_general(mix, flat, (((0,), (0,)), ((), ())), preferred_element_type=jnp.float32)


def per_device(
    residual_in,
    conv_input,
    input_gate,
    output_gate,
    conv_taps,
    doc_ids,
    proj_weight,
    norm_gain,
    expert_ids,
    expert_weight,
    w_gate,
    w_up,
    w_down,
):
    kernel_width = conv_taps.shape[0]
    rim_rows = kernel_width - 1
    devices = lax.axis_size("sp")
    half = devices // 2
    local_experts = w_gate.shape[0]
    half_experts = half * local_experts
    first = (lax.axis_index("sp") // half) * half_experts

    ids = expert_ids.T
    weights = expert_weight.T
    routes = jnp.concatenate([ids.astype(jnp.float32), weights], axis=0)
    far_routes = to_mirror(routes)
    far_ids = far_routes[:2].astype(jnp.int32)
    far_weights = far_routes[2:]

    product = input_gate.astype(jnp.float32) * conv_input.astype(jnp.float32)
    doc_float = doc_ids.astype(jnp.float32)
    doc_rim = jnp.broadcast_to(doc_float[-rim_rows:, None], (rim_rows, 128))
    rim = from_behind(jnp.concatenate([product[-rim_rows:], doc_rim], axis=1), "sp", 1)
    channels = product.shape[1]
    prev_in, prev_ids = rim[:, :channels], rim[:, channels]
    padded_in = jnp.concatenate([prev_in, product], axis=0)
    padded_ids = jnp.concatenate([prev_ids, doc_float], axis=0)
    length = product.shape[0]
    conv_sum = jnp.zeros(product.shape, jnp.float32)
    for offset in range(kernel_width):
        same_doc = padded_ids[offset : offset + length] == doc_float
        term = conv_taps[offset].astype(jnp.float32)[None, :] * padded_in[offset : offset + length]
        conv_sum = conv_sum + jnp.where(same_doc[:, None], term, 0.0)
    gated = (output_gate.astype(jnp.float32) * conv_sum).astype(jnp.bfloat16)
    regrouped = lax.all_to_all(gated, "tp", split_axis=0, concat_axis=1, tiled=True)

    pick, mix = slot_matrices(ids, weights, first, half_experts)
    far_pick, far_mix = slot_matrices(far_ids, far_weights, first, half_experts)

    mixed = jnp.dot(regrouped, proj_weight, preferred_element_type=jnp.float32)
    hidden = residual_in.astype(jnp.float32) + mixed
    scale_rows = lax.rsqrt(jnp.mean(hidden * hidden, axis=-1, keepdims=True) + epsilon)
    normed = (hidden * scale_rows * norm_gain[None, :]).astype(jnp.bfloat16)
    width = normed.shape[1] // CHUNKS

    far_rows = [to_mirror(normed[:, c * width : (c + 1) * width]) for c in range(CHUNKS)]
    own_slots = within_half(pack(pick, normed, half, local_experts))
    own_slots, far_rows[0] = lax.optimization_barrier((own_slots, far_rows[0]))
    far_slots = [within_half(pack(far_pick, far_rows[0], half, local_experts))]
    own_slots, far_slots[0] = lax.optimization_barrier((own_slots, far_slots[0]))
    own_out = expert_ffn([own_slots], w_gate, w_up, w_down)[0]
    own_out, *rest = lax.optimization_barrier((own_out, *far_rows[1:]))
    far_slots += [within_half(pack(far_pick, rows, half, local_experts)) for rows in rest]

    far_out = list(expert_ffn(far_slots, w_gate, w_up, w_down))
    far_sums = []
    for c in range(CHUNKS):
        back = within_half(far_out[c])
        if c + 1 < CHUNKS:
            back, far_out[c + 1] = lax.optimization_barrier((back, far_out[c + 1]))
        else:
            back, own_out = lax.optimization_barrier((back, own_out))
        far_sums.append(to_mirror(unpack(far_mix, back).astype(jnp.bfloat16)))
    total = hidden + unpack(mix, within_half(own_out))
    return (total + jnp.concatenate(far_sums, axis=1).astype(jnp.float32)).astype(jnp.bfloat16)


def solution(mesh):
    return jax.shard_map(
        per_device,
        mesh=mesh,
        in_specs=(
            P(("sp", "tp"), None),
            P("sp", "tp"),
            P("sp", "tp"),
            P("sp", "tp"),
            P(None, "tp"),
            P("sp"),
            P(),
            P(),
            P(("sp", "tp"), None),
            P(("sp", "tp"), None),
            P("sp", None, None),
            P("sp", None, None),
            P("sp", None, None),
        ),
        out_specs=P(("sp", "tp"), None),
        check_vma=False,
    )
```

```python
import functools

import jax
import jax.numpy as jnp
from jax import lax
from jax.experimental import pallas as pl
from jax.sharding import PartitionSpec as P


CAP = 64
epsilon = 1e-06


def from_behind(x, axis, by):
    devices = lax.axis_size(axis)
    pairs = [(i, i + by) for i in range(devices) if 0 <= i + by < devices]
    return lax.ppermute(x, axis, pairs)


def to_mirror(x):
    devices = lax.axis_size("sp")
    pairs = [(i, (i + devices // 2) % devices) for i in range(devices)]
    return lax.ppermute(x, "sp", pairs)


def within_half(x):
    devices = lax.axis_size("sp")
    half = devices // 2
    groups = [list(range(half)), list(range(half, devices))]
    return lax.all_to_all(x, "sp", split_axis=0, concat_axis=0, axis_index_groups=groups, tiled=True)


def ffn_kernel(blocks, *refs):
    x_refs = refs[:blocks]
    gate_ref, up_ref, down_ref = refs[blocks : blocks + 3]
    out_refs = refs[blocks + 3 :]
    peers, cap, width = x_refs[0].shape
    count = peers * cap
    rows = jnp.concatenate([x_ref[...].reshape(count, width) for x_ref in x_refs], axis=0)
    gate_val = jnp.dot(rows, gate_ref[...], preferred_element_type=jnp.float32)
    up_val = jnp.dot(rows, up_ref[...], preferred_element_type=jnp.float32)
    act = (gate_val * jax.nn.sigmoid(gate_val) * up_val).astype(jnp.bfloat16)
    out = jnp.dot(act, down_ref[...], preferred_element_type=jnp.float32).astype(jnp.bfloat16)
    for b in range(blocks):
        out_refs[b][...] = out[b * count : (b + 1) * count].reshape(peers, cap, width)


def expert_ffn(xs, w_gate, w_up, w_down):
    blocks = len(xs)
    peers, experts, cap, model = xs[0].shape
    hidden = w_gate.shape[2]
    row_spec = pl.BlockSpec((peers, None, cap, model), lambda e: (0, e, 0, 0))
    return pl.pallas_call(
        functools.partial(ffn_kernel, blocks),
        grid=(experts,),
        in_specs=[row_spec] * blocks
        + [
            pl.BlockSpec((None, model, hidden), lambda e: (e, 0, 0)),
            pl.BlockSpec((None, model, hidden), lambda e: (e, 0, 0)),
            pl.BlockSpec((None, hidden, model), lambda e: (e, 0, 0)),
        ],
        out_specs=[row_spec] * blocks,
        out_shape=[jax.ShapeDtypeStruct(xs[0].shape, jnp.bfloat16)] * blocks,
        cost_estimate=pl.CostEstimate(
            flops=6 * blocks * experts * peers * cap * model * hidden,
            bytes_accessed=2 * (w_gate.size + w_up.size + w_down.size + 2 * blocks * xs[0].size),
            transcendentals=blocks * experts * peers * cap * hidden,
        ),
    )(*xs, w_gate, w_up, w_down)


def slot_matrices(ids, weights, first, experts):
    tokens = ids.shape[1]
    local = ids - first
    names = jnp.arange(experts, dtype=jnp.int32)[:, None]
    hits = [local[r][None, :] == names for r in range(2)]
    named = (hits[0] | hits[1]).astype(jnp.bfloat16)
    at = jnp.arange(tokens, dtype=jnp.int32)
    earlier = (at[:, None] < at[None, :]).astype(jnp.bfloat16)
    before = jnp.dot(named, earlier, preferred_element_type=jnp.float32)
    slots = jnp.arange(experts * CAP, dtype=jnp.int32)[:, None]
    pick, mix = False, 0.0
    for r in range(2):
        rank = jnp.sum(jnp.where(hits[r], before, 0.0), axis=0).astype(jnp.int32)
        match = slots == (local[r] * CAP + rank)[None, :]
        pick = pick | match
        mix = mix + jnp.where(match, weights[r][None, :], 0.0)
    return pick.astype(jnp.bfloat16), mix.astype(jnp.bfloat16)


def pack(pick, rows, peers, experts):
    out = jnp.dot(pick, rows, preferred_element_type=jnp.float32).astype(jnp.bfloat16)
    return out.reshape(peers, experts, CAP, rows.shape[1])


def unpack(mix, returned):
    flat = returned.reshape(-1, returned.shape[-1])
    return lax.dot_general(mix, flat, (((0,), (0,)), ((), ())), preferred_element_type=jnp.float32)


def per_device(
    residual_in,
    conv_input,
    input_gate,
    output_gate,
    conv_taps,
    doc_ids,
    proj_weight,
    norm_gain,
    expert_ids,
    expert_weight,
    w_gate,
    w_up,
    w_down,
):
    kernel_width = conv_taps.shape[0]
    rim_rows = kernel_width - 1
    devices = lax.axis_size("sp")
    half = devices // 2
    local_experts = w_gate.shape[0]
    half_experts = half * local_experts
    first = (lax.axis_index("sp") // half) * half_experts

    ids = expert_ids.T
    weights = expert_weight.T
    routes = jnp.concatenate([ids.astype(jnp.float32), weights], axis=0)
    far_routes = to_mirror(routes)

    product = input_gate.astype(jnp.float32) * conv_input.astype(jnp.float32)
    doc_float = doc_ids.astype(jnp.float32)
    doc_rim = jnp.broadcast_to(doc_float[-rim_rows:, None], (rim_rows, 128))
    rim = from_behind(jnp.concatenate([product[-rim_rows:], doc_rim], axis=1), "sp", 1)
    channels = product.shape[1]
    prev_in, prev_ids = rim[:, :channels], rim[:, channels]
    padded_in = jnp.concatenate([prev_in, product], axis=0)
    padded_ids = jnp.concatenate([prev_ids, doc_float], axis=0)
    length = product.shape[0]
    conv_sum = jnp.zeros(product.shape, jnp.float32)
    for offset in range(kernel_width):
        same_doc = padded_ids[offset : offset + length] == doc_float
        term = conv_taps[offset].astype(jnp.float32)[None, :] * padded_in[offset : offset + length]
        conv_sum = conv_sum + jnp.where(same_doc[:, None], term, 0.0)
    gated = (output_gate.astype(jnp.float32) * conv_sum).astype(jnp.bfloat16)
    regrouped = lax.all_to_all(gated, "tp", split_axis=0, concat_axis=1, tiled=True)

    regrouped, far_routes = lax.optimization_barrier((regrouped, far_routes))
    far_ids = far_routes[:2].astype(jnp.int32)
    far_weights = far_routes[2:]
    pick, mix = slot_matrices(ids, weights, first, half_experts)
    far_pick, far_mix = slot_matrices(far_ids, far_weights, first, half_experts)

    mixed = jnp.dot(regrouped, proj_weight, preferred_element_type=jnp.float32)
    hidden = residual_in.astype(jnp.float32) + mixed
    scale_rows = lax.rsqrt(jnp.mean(hidden * hidden, axis=-1, keepdims=True) + epsilon)
    normed = (hidden * scale_rows * norm_gain[None, :]).astype(jnp.bfloat16)

    far_rows = to_mirror(normed)
    own_slots = within_half(pack(pick, normed, half, local_experts))
    own_slots, far_rows = lax.optimization_barrier((own_slots, far_rows))
    far_slots = within_half(pack(far_pick, far_rows, half, local_experts))
    own_out, far_out = expert_ffn([own_slots, far_slots], w_gate, w_up, w_down)
    far_part = unpack(far_mix, within_half(far_out)).astype(jnp.bfloat16)
    far_part, own_out = lax.optimization_barrier((far_part, own_out))
    far_sum = to_mirror(far_part)
    total = hidden + unpack(mix, within_half(own_out))
    return (total + far_sum.astype(jnp.float32)).astype(jnp.bfloat16)


def solution(mesh):
    return jax.shard_map(
        per_device,
        mesh=mesh,
        in_specs=(
            P(("sp", "tp"), None),
            P("sp", "tp"),
            P("sp", "tp"),
            P("sp", "tp"),
            P(None, "tp"),
            P("sp"),
            P(),
            P(),
            P(("sp", "tp"), None),
            P(("sp", "tp"), None),
            P("sp", None, None),
            P("sp", None, None),
            P("sp", None, None),
        ),
        out_specs=P(("sp", "tp"), None),
        check_vma=False,
    )
```
